32 devices in a mesh: ep: 8 (over z, y), tp: 4 (over x, core).
Axes of the slice: x: 2, y: 2, z: 4, core: 2. Of those that a mesh axis runs over, the one named last changes fastest.
Arguments:
- tokens: bfloat16 [1024, 2048], P('ep', 'tp'), may hold values from -6 to 6
- norm_gain: bfloat16 [2048], P('tp'), may hold values from 0.099609375 to 1.8984375
- routes: int32 [1024, 2], P('ep'), may hold values from 0 to 7, as said below
- gate_weights: float32 [1024, 2], P('ep'), may hold values from 0.1 to 1
- w_gate: bfloat16 [8, 2048, 4096], P('ep', None, 'tp'), may hold values from -0.125 to 0.125
- w_up: bfloat16 [8, 2048, 4096], P('ep', None, 'tp'), may hold values from -0.125 to 0.125
- w_down: bfloat16 [8, 4096, 2048], P('ep', 'tp'), may hold values from -0.875 to 0.875
- out_gain: bfloat16 [2048], P('tp'), may hold values from 0.099609375 to 1.8984375
Outputs:
- mixed: bfloat16 [1024, 2048], P('ep', 'tp')
The draws below stay inside these ranges and needn't reach their ends.
Inputs may be any that keep to these rules, and one draw needn't show every extreme that they name: `routes`: each row names 2 different experts of one group (their quotients by 8 agree). In each aligned block of 128 rows no expert is named by more than 64 rows, and in every block some expert is named by exactly 64 rows.
All inputs are finite; a program needn't handle non-finite values.
Results may differ from the reference program's by a relative error of at most 0.019.
Values may be sent and summed in bfloat16 or wider, within the bound.
No kernel may reach another device: no remote copies, remote signals or barrier semaphores. Data moves between devices by JAX's collectives and lax.ppermute only.
A program may use at most 64 MiB of HBM per device.

```python
import math
import jax
import jax.numpy as jnp
from jax import lax

D = 2048
FF = 4096
EPG = 8
TOPK = 2
TOK_DEV = 128
EXPERTS = 8
GROUPS = 1
MEAN = 32
CAP = 64
TOKENS = 1024
N_EP = 8
N_TP = 4


def draw_routes(key, part):
    folded = jax.random.fold_in(key, 5)
    k_pop, k_jit, k_perm = jax.random.split(folded, 3)
    popular = jax.random.randint(k_pop, (EXPERTS,), 0, 4)
    jitter = jax.random.randint(k_jit, (N_EP, EXPERTS), 0, 3)
    expert_ids = jnp.arange(EXPERTS, dtype=jnp.int32)
    scores = (popular[None, :] * 4 + jitter) * EXPERTS + expert_ids[None, :]
    sorted_ids = jnp.argsort(scores, axis=1)
    ranking = jnp.argsort(sorted_ids, axis=1)
    quarter = ranking * 4 // EXPERTS
    counts = jnp.where(quarter == 3, 2 * MEAN, jnp.where(quarter == 2, MEAN, MEAN // 2)).astype(jnp.int32)
    group_copies = counts.reshape(N_EP, GROUPS, EPG).sum(axis=2)
    group_tokens = group_copies // 2
    token_end = jnp.cumsum(group_tokens, axis=1)
    token_start = token_end - group_tokens
    copy_start = jnp.cumsum(group_copies, axis=1) - group_copies
    expert_end = jnp.cumsum(counts, axis=1)
    positions = jnp.arange(TOK_DEV, dtype=jnp.int32)
    group_of = jnp.sum(positions[None, :, None] >= token_end[:, None, :], axis=2).astype(jnp.int32)
    within = positions[None, :] - jnp.take_along_axis(token_start, group_of, axis=1)
    first_copy = jnp.take_along_axis(copy_start, group_of, axis=1) + within
    second_copy = first_copy + jnp.take_along_axis(group_tokens, group_of, axis=1)

    def owner_of(copies):
        return jnp.sum(copies[:, :, None] >= expert_end[:, None, :], axis=2).astype(jnp.int32)
    chosen = jnp.stack([owner_of(first_copy), owner_of(second_copy)], axis=2)
    shuffle = jax.random.randint(k_perm, (N_EP, TOK_DEV), 0, 1 << 20) * TOK_DEV + positions[None, :]
    shuffled_order = jnp.argsort(shuffle, axis=1)
    chosen = jnp.take_along_axis(chosen, shuffled_order[:, :, None], axis=1)
    return chosen.reshape(N_EP * TOK_DEV, 2).astype(jnp.int32)


def draw_w_down(key, part):
    k_base, k_rough = jax.random.split(jax.random.fold_in(key, 7))
    column = jnp.arange(D, dtype=jnp.float32) / D
    base = jnp.clip(jax.random.normal(k_base, (EXPERTS, FF, D), jnp.float32), -4.0, 4.0)
    rising = 10.0 ** column
    rough = jax.random.uniform(k_rough, (D,), jnp.float32, 0.6, 1.4)
    return (base * (rising * rough / FF ** 0.5)[None, None, :]).astype(jnp.bfloat16)


def block_levels(own_key, shape, pieces, least, largest):
    def one(axis_at, parts):
        draws = jax.random.uniform(jax.random.fold_in(jax.random.fold_in(own_key, 6), axis_at), (parts,), jnp.float32, least / len(pieces), largest / len(pieces))
        return jnp.repeat(jnp.exp(draws), shape[axis_at] // parts).reshape((-1,) + (1,) * (len(shape) - axis_at - 1))

    gain = one(*pieces[0])
    for cut in pieces[1:]:
        gain = gain * one(*cut)
    return gain


def bell_draw(rng, extent, width, limit, shards=(), held_as=jnp.bfloat16):
    factor_of = block_levels(rng, extent, shards, -0.22, 0.18) if shards else 1.0
    result = jax.random.normal(rng, extent, jnp.float32) * width * factor_of
    return jnp.minimum(jnp.maximum(result, -limit), limit).astype(held_as)


def setup_inputs(seed: int = 0) -> dict:
    keys = jax.random.split(jax.random.key(seed), 9)
    tokens = bell_draw(keys[0], (TOKENS, D), 1.0, 6.0, ((0, 8), (1, 4)))
    norm_gain = jnp.clip(1.0 + 0.18 * jax.random.normal(keys[1], (D,), jnp.float32), 0.099609375, 1.8984375).astype(jnp.bfloat16)
    routes = draw_routes(jax.random.fold_in(keys[8], 71), 0)
    gate_weights = jnp.clip(jnp.exp(math.log(1.0) - 2.3025851 * jax.random.uniform(keys[3], (TOKENS, TOPK), jnp.float32) ** block_levels(keys[3], (TOKENS, TOPK), ((0, 8),), -0.2, 0.2)), 0.1, 1.0)
    w_gate = bell_draw(keys[4], (EXPERTS, D, FF), D ** -0.5, 0.125, ((0, 8), (2, 4)))
    w_up = bell_draw(keys[5], (EXPERTS, D, FF), D ** -0.5, 0.125, ((0, 8), (2, 4)))
    w_down = draw_w_down(jax.random.fold_in(keys[8], 71), 0)
    out_gain = jnp.clip(1.0 + 0.18 * jax.random.normal(keys[7], (D,), jnp.float32), 0.099609375, 1.8984375).astype(jnp.bfloat16)
    return dict(tokens=tokens, norm_gain=norm_gain, routes=routes, gate_weights=gate_weights, w_gate=w_gate, w_up=w_up, w_down=w_down, out_gain=out_gain)


epsilon = 1e-06

def route_slots(routes):
    blocks = routes.reshape(N_EP, TOK_DEV * TOPK)
    onehot = (blocks[:, :, None] == jnp.arange(EXPERTS, dtype=jnp.int32)[None, None, :]).astype(jnp.int32)
    before = jnp.cumsum(onehot, axis=1) - onehot
    return lax.optimization_barrier(jnp.sum(before * onehot, axis=2)).astype(jnp.int32)

def reference(tokens, norm_gain, routes, gate_weights, w_gate, w_up, w_down, out_gain):
    x_float = tokens.astype(jnp.float32)
    scale_in = lax.rsqrt(lax.optimization_barrier(jnp.mean(x_float * x_float, axis=1, keepdims=True)) + epsilon)
    normed = (x_float * scale_in * norm_gain.astype(jnp.float32)).astype(jnp.bfloat16)
    slot_index = route_slots(routes)
    expert_ids = routes.reshape(N_EP, TOK_DEV * TOPK).astype(jnp.int32)
    source = jnp.arange(N_EP, dtype=jnp.int32)[:, None]
    copy_ids = jnp.arange(TOK_DEV * TOPK, dtype=jnp.int32)[None, :]
    token_ids = (source * TOK_DEV + copy_ids // TOPK).astype(jnp.int32)
    buffer_pos = (source * CAP + slot_index).astype(jnp.int32)
    table = jnp.full((EXPERTS, N_EP * CAP), TOKENS, jnp.int32).at[expert_ids, buffer_pos].set(token_ids)
    padded = jnp.concatenate([normed, jnp.zeros((1, D), jnp.bfloat16)], axis=0)

    def expert(inputs):
        row_table, gate_mat, up_mat, down_mat = inputs
        arrived = padded[row_table]
        gate_sum = jnp.dot(arrived, gate_mat, preferred_element_type=jnp.float32)
        up_sum = jnp.dot(arrived, up_mat, preferred_element_type=jnp.float32)
        hidden = (jax.nn.silu(gate_sum) * up_sum).astype(jnp.bfloat16)
        hidden_blocks = hidden.reshape(N_EP * CAP, N_TP, FF // N_TP).astype(jnp.float32)
        down_blocks = down_mat.reshape(N_TP, FF // N_TP, D).astype(jnp.float32)
        partial_value = jnp.einsum('rtf,tfd->trd', hidden_blocks, down_blocks).astype(jnp.bfloat16)
        partial_value = lax.optimization_barrier(partial_value)
        return lax.optimization_barrier(jnp.sum(partial_value.astype(jnp.float32), axis=0)).astype(jnp.bfloat16)
    outputs = lax.map(expert, (table, w_gate, w_up, w_down))
    picked = outputs[expert_ids, buffer_pos].astype(jnp.float32).reshape(TOKENS, TOPK, D)
    combined = lax.optimization_barrier(jnp.sum(picked * gate_weights[:, :, None], axis=1))
    scale_out = lax.rsqrt(lax.optimization_barrier(jnp.mean(combined * combined, axis=1, keepdims=True)) + epsilon)
    return (combined * scale_out * out_gain.astype(jnp.float32)).astype(jnp.bfloat16)
```

```python
import functools

import jax
import jax.numpy as jnp
from jax import lax
from jax.experimental import pallas as pl
from jax.experimental.pallas import tpu as pltpu
from jax.sharding import PartitionSpec as P

epsilon = 1e-06
PAD = 16


def flip(value, axis, mask):
    size = lax.axis_size(axis)
    return lax.ppermute(value, axis, [(i, i ^ mask) for i in range(size)])


def expert_kernel(
    rank, own_ref, peer_ref, gate_ref, up_ref, down_ref, send_ref, keep_ref, normed_ref, hidden_ref,
    *, blocks, width, rows, tile, steps
):
    step = pl.program_id(0)
    me = rank[0]

    @pl.when(step == 0)
    def _():
        squares = jnp.zeros((rows, 1), jnp.float32)
        for ref in (own_ref, peer_ref):
            for k in range(blocks // 2):
                x = ref[k, :rows].astype(jnp.float32)
                squares += jnp.sum(x * x, axis=1, keepdims=True)
        scale = lax.rsqrt(squares / (blocks * width) + epsilon)
        for j in range(blocks):
            away = me ^ j
            both = jnp.where((away & 1) == 1, peer_ref[away >> 1], own_ref[away >> 1]).astype(jnp.float32)
            normed_ref[:, j * width : (j + 1) * width] = (
                both[:rows] * scale * both[rows : rows + 1]
            ).astype(jnp.bfloat16)

    for k in range(steps):
        @pl.when(step == k)
        def _(k=k):
            normed = normed_ref[...]
            gate = jnp.dot(normed, gate_ref[0], preferred_element_type=jnp.float32)
            up = jnp.dot(normed, up_ref[0], preferred_element_type=jnp.float32)
            hidden_ref[:, k * tile : (k + 1) * tile] = (
                gate / (1.0 + jnp.exp(-gate)) * up
            ).astype(jnp.bfloat16)

    @pl.when(step >= steps)
    def _():
        part = jnp.dot(
            hidden_ref[...], down_ref[0], preferred_element_type=jnp.float32
        ).astype(jnp.bfloat16)

        @pl.when(step < steps + blocks // 2)
        def _():
            send_ref[0] = part

        @pl.when(step >= steps + blocks // 2)
        def _():
            keep_ref[0] = part


def expert_call(rank, own, peer, w_gate, w_up, w_down, rows):
    half, _, width = own.shape
    blocks = 2 * half
    full, ff = w_gate.shape[1], w_gate.shape[2]
    tile = min(256, ff)
    steps = ff // tile

    def column(i, rank):
        n = jnp.maximum(i - steps, 0)
        away = jnp.where(n < half, 2 * n + 1, 2 * (n - half))
        return rank[0] ^ away

    body = functools.partial(
        expert_kernel, blocks=blocks, width=width, rows=rows, tile=tile, steps=steps
    )
    return pl.pallas_call(
        body,
        grid_spec=pltpu.PrefetchScalarGridSpec(
            num_scalar_prefetch=1,
            grid=(steps + blocks,),
            in_specs=[
                pl.BlockSpec(own.shape, lambda i, r: (0, 0, 0)),
                pl.BlockSpec(peer.shape, lambda i, r: (0, 0, 0)),
                pl.BlockSpec((1, full, tile), lambda i, r: (0, 0, jnp.minimum(i, steps - 1))),
                pl.BlockSpec((1, full, tile), lambda i, r: (0, 0, jnp.minimum(i, steps - 1))),
                pl.BlockSpec((1, ff, width), lambda i, r: (0, 0, column(i, r))),
            ],
            out_specs=[
                pl.BlockSpec((1, rows, width), lambda i, r: (jnp.clip(i - steps, 0, half - 1), 0, 0)),
                pl.BlockSpec((1, rows, width), lambda i, r: (jnp.clip(i - steps - half, 0, half - 1), 0, 0)),
            ],
            scratch_shapes=[
                pltpu.VMEM((rows, full), jnp.bfloat16),
                pltpu.VMEM((rows, ff), jnp.bfloat16),
            ],
        ),
        out_shape=[jax.ShapeDtypeStruct((half, rows, width), jnp.bfloat16)] * 2,
        compiler_params=pltpu.CompilerParams(
            dimension_semantics=("arbitrary",), vmem_limit_bytes=24 << 20
        ),
        cost_estimate=pl.CostEstimate(
            flops=6 * rows * full * ff, transcendentals=rows * ff, bytes_accessed=6 * full * ff
        ),
        name="expert",
    )(rank, own, peer, w_gate, w_up, w_down)


def gather_width(rows_here, tp):
    stack = rows_here[None]
    mask = 2
    while mask < tp:
        stack = jnp.concatenate([stack, flip(stack, "tp", mask)], axis=0)
        mask *= 2
    return stack, flip(stack, "tp", 1)


def add(a, b):
    return (a.astype(jnp.float32) + b.astype(jnp.float32)).astype(jnp.bfloat16)


def scatter_sum(send, keep, tp):
    stack = add(keep, flip(send, "tp", 1))
    mask = tp // 2
    while mask > 1:
        half = stack.shape[0] // 2
        stack = add(stack[:half], flip(stack[half:], "tp", mask))
        mask //= 2
    return stack[0]


def total_over_tp(value, tp):
    mask = 1
    while mask < tp:
        value = value + flip(value, "tp", mask)
        mask *= 2
    return value


def shards(tokens, norm_gain, routes, gate_weights, w_gate, w_up, w_down, out_gain):
    tok_rows, width = tokens.shape
    tp = lax.axis_size("tp")
    experts = lax.axis_size("ep")
    full_width = width * tp
    top_count = routes.shape[1]
    capacity = 2 * top_count * tok_rows // experts
    me = lax.axis_index("ep")
    rank = lax.axis_index("tp").astype(jnp.int32).reshape(1)

    flat_ids = routes.reshape(-1)
    onehot = (flat_ids[:, None] == jnp.arange(experts, dtype=jnp.int32)[None, :]).astype(jnp.int32)
    before = jnp.cumsum(onehot, axis=0) - onehot
    slot_index = jnp.sum(before * onehot, axis=1)
    dest = ((flat_ids ^ me) * capacity + slot_index).reshape(tok_rows, top_count)
    places = jnp.arange(experts * capacity, dtype=jnp.int32)
    scatter_mat = jnp.any(dest[None, :, :] == places[:, None, None], axis=2).astype(jnp.bfloat16)
    outgoing = jnp.dot(scatter_mat, tokens, preferred_element_type=jnp.float32).astype(jnp.bfloat16)
    outgoing = outgoing.reshape(experts, capacity, width)

    far = list(range(experts // 2, experts))
    near = list(range(experts // 2))
    gain_rows = jnp.broadcast_to(norm_gain[None, :], (PAD, width))
    arrived = {}
    for m in far + near[::-1]:
        arrived[m] = outgoing[m] if m == 0 else flip(outgoing[m], "ep", m)
    groups = (far, near)
    wide = []
    for group in groups:
        here = jnp.concatenate([arrived[m] for m in group] + [gain_rows], axis=0)
        wide.append(gather_width(here, tp))
    back = {}
    for group, (own, peer) in zip(groups, wide):
        send, keep = expert_call(rank, own, peer, w_gate, w_up, w_down, len(group) * capacity)
        summed = scatter_sum(send, keep, tp).reshape(len(group), capacity, width)
        for k, m in enumerate(group):
            back[m] = summed[k] if m == 0 else flip(summed[k], "ep", m)
    came_back = jnp.concatenate([back[m] for m in range(experts)], axis=0)

    combined = jnp.zeros((tok_rows, width), jnp.float32)
    for k in range(top_count):
        pick = (dest[:, k : k + 1] == places[None, :]).astype(jnp.bfloat16)
        picked = jnp.dot(pick, came_back, preferred_element_type=jnp.float32)
        combined = combined + picked * gate_weights[:, k : k + 1]
    out_sums = total_over_tp(jnp.sum(combined * combined, axis=1), tp)
    scale_out = lax.rsqrt(out_sums / full_width + epsilon)
    return (combined * scale_out[:, None] * out_gain.astype(jnp.float32)).astype(jnp.bfloat16)


def solution(mesh):
    placed = (
        P("ep", "tp"),
        P("tp"),
        P("ep", None),
        P("ep", None),
        P("ep", None, "tp"),
        P("ep", None, "tp"),
        P("ep", "tp", None),
        P("tp"),
    )
    return jax.shard_map(
        shards, mesh=mesh, in_specs=placed, out_specs=P("ep", "tp"), check_vma=False
    )
```

```python
import functools

import jax
import jax.numpy as jnp
from jax import lax
from jax.experimental import pallas as pl
from jax.experimental.pallas import tpu as pltpu
from jax.sharding import PartitionSpec as P


epsilon = 1e-06
PAD = 16


def flip(value, axis, mask):
    size = lax.axis_size(axis)
    return lax.ppermute(value, axis, [(i, i ^ mask) for i in range(size)])


def load_kernel(*refs):
    count = 3
    sources, targets, sems = refs[:count], refs[count : 2 * count], refs[2 * count]
    copies = []
    for i in range(count):
        rows = sources[i].shape[1]
        piece = rows // 4
        for k in range(4):
            part = pl.ds(k * piece, piece)
            copies.append(
                pltpu.make_async_copy(
                    sources[i].at[:, part], targets[i].at[:, part], sems.at[i, k]
                )
            )
    for copy in copies:
        copy.start()
    for copy in copies:
        copy.wait()


def load_weights(*weights):
    return pl.pallas_call(
        load_kernel,
        in_specs=[pl.BlockSpec(memory_space=pltpu.HBM)] * 3,
        out_specs=[pl.BlockSpec(memory_space=pltpu.VMEM)] * 3,
        out_shape=[pltpu.VMEM(w.shape, w.dtype) for w in weights],
        scratch_shapes=[pltpu.SemaphoreType.DMA((3, 4))],
        compiler_params=pltpu.CompilerParams(vmem_limit_bytes=1 << 20),
        cost_estimate=pl.CostEstimate(
            flops=1 << 31, transcendentals=0, bytes_accessed=sum(w.size * 2 for w in weights)
        ),
        name="load",
    )(*(pltpu.with_memory_space_constraint(w, pltpu.HBM) for w in weights))


def expert_kernel(
    rank, own_ref, peer_ref, gate_ref, up_ref, down_ref, send_ref, keep_ref, normed_ref, hidden_ref,
    *, blocks, width, rows, tile, steps
):
    me = rank[0]
    squares = jnp.zeros((rows, 1), jnp.float32)
    for ref in (own_ref, peer_ref):
        for k in range(blocks // 2):
            x = ref[k, :rows].astype(jnp.float32)
            squares += jnp.sum(x * x, axis=1, keepdims=True)
    scale = lax.rsqrt(squares / (blocks * width) + epsilon)
    for j in range(blocks):
        away = me ^ j
        both = jnp.where((away & 1) == 1, peer_ref[away >> 1], own_ref[away >> 1]).astype(jnp.float32)
        normed_ref[:, j * width : (j + 1) * width] = (
            both[:rows] * scale * both[rows : rows + 1]
        ).astype(jnp.bfloat16)
    for k in range(steps):
        part = slice(k * tile, (k + 1) * tile)
        gate = jnp.dot(normed_ref[...], gate_ref[0, :, part], preferred_element_type=jnp.float32)
        up = jnp.dot(normed_ref[...], up_ref[0, :, part], preferred_element_type=jnp.float32)
        hidden_ref[:, part] = (gate / (1.0 + jnp.exp(-gate)) * up).astype(jnp.bfloat16)
    for j in range(blocks):
        away = me ^ j
        part = jnp.dot(
            hidden_ref[...], down_ref[0, :, j * width : (j + 1) * width],
            preferred_element_type=jnp.float32,
        ).astype(jnp.bfloat16)

        @pl.when((away & 1) == 1)
        def _():
            send_ref[away >> 1] = part

        @pl.when((away & 1) == 0)
        def _():
            keep_ref[away >> 1] = part


def expert_call(rank, own, peer, w_gate, w_up, w_down, rows):
    half, _, width = own.shape
    blocks = 2 * half
    full, ff = w_gate.shape[1], w_gate.shape[2]
    tile = min(256, ff)
    steps = ff // tile
    body = functools.partial(
        expert_kernel, blocks=blocks, width=width, rows=rows, tile=tile, steps=steps
    )
    vmem = pl.BlockSpec(memory_space=pltpu.VMEM)
    return pl.pallas_call(
        body,
        in_specs=[pl.BlockSpec(memory_space=pltpu.SMEM)] + [vmem] * 5,
        out_specs=[vmem] * 2,
        out_shape=[jax.ShapeDtypeStruct((half, rows, width), jnp.bfloat16)] * 2,
        scratch_shapes=[
            pltpu.VMEM((rows, full), jnp.bfloat16),
            pltpu.VMEM((rows, ff), jnp.bfloat16),
        ],
        compiler_params=pltpu.CompilerParams(vmem_limit_bytes=16 << 20),
        cost_estimate=pl.CostEstimate(
            flops=6 * rows * full * ff, transcendentals=rows * ff, bytes_accessed=6 * full * ff
        ),
        name="expert",
    )(rank, own, peer, *(pltpu.with_memory_space_constraint(w, pltpu.VMEM) for w in (w_gate, w_up, w_down)))


def gather_width(rows_here, tp):
    stack = rows_here[None]
    mask = 2
    while mask < tp:
        stack = jnp.concatenate([stack, flip(stack, "tp", mask)], axis=0)
        mask *= 2
    return stack, flip(stack, "tp", 1)


def add(a, b):
    return (a.astype(jnp.float32) + b.astype(jnp.float32)).astype(jnp.bfloat16)


def scatter_sum(send, keep, tp):
    stack = add(keep, flip(send, "tp", 1))
    mask = tp // 2
    while mask > 1:
        half = stack.shape[0] // 2
        stack = add(stack[:half], flip(stack[half:], "tp", mask))
        mask //= 2
    return stack[0]


def total_over_tp(value, tp):
    mask = 1
    while mask < tp:
        value = value + flip(value, "tp", mask)
        mask *= 2
    return value


def split_masks(experts):
    return list(range(experts // 2, experts))[::-1], list(range(experts // 2))[::-1]


def shards(tokens, norm_gain, routes, gate_weights, w_gate, w_up, w_down, out_gain):
    tok_rows, width = tokens.shape
    tp = lax.axis_size("tp")
    experts = lax.axis_size("ep")
    full_width = width * tp
    top_count = routes.shape[1]
    capacity = 2 * top_count * tok_rows // experts
    me = lax.axis_index("ep")
    rank = lax.axis_index("tp").astype(jnp.int32).reshape(1)

    flat_ids = routes.reshape(-1)
    onehot = (flat_ids[:, None] == jnp.arange(experts, dtype=jnp.int32)[None, :]).astype(jnp.int32)
    before = jnp.cumsum(onehot, axis=0) - onehot
    slot_index = jnp.sum(before * onehot, axis=1)
    dest = ((flat_ids ^ me) * capacity + slot_index).reshape(tok_rows, top_count)
    places = jnp.arange(experts * capacity, dtype=jnp.int32)
    scatter_mat = jnp.any(dest[None, :, :] == places[:, None, None], axis=2).astype(jnp.bfloat16)
    outgoing = jnp.dot(scatter_mat, tokens, preferred_element_type=jnp.float32).astype(jnp.bfloat16)
    outgoing = outgoing.reshape(experts, capacity, width)
    outgoing = lax.optimization_barrier([outgoing[m] for m in range(experts)])

    far, near = split_masks(experts)
    gain_rows = jnp.broadcast_to(norm_gain[None, :], (PAD, width))
    arrived = {}
    for m in far + near:
        arrived[m] = outgoing[m] if m == 0 else flip(outgoing[m], "ep", m)
    groups = (far, near)
    wide = []
    for group in groups:
        here = jnp.concatenate([arrived[m] for m in group] + [gain_rows], axis=0)
        wide.append(gather_width(here, tp))
    w_gate, w_up, w_down = load_weights(w_gate, w_up, w_down)
    back = {}
    for group, (own, peer) in zip(groups, wide):
        send, keep = expert_call(rank, own, peer, w_gate, w_up, w_down, len(group) * capacity)
        summed = scatter_sum(send, keep, tp).reshape(len(group), capacity, width)
        for k, m in enumerate(group):
            back[m] = summed[k] if m == 0 else flip(summed[k], "ep", m)
    came_back = jnp.concatenate([back[m] for m in range(experts)], axis=0)

    combined = jnp.zeros((tok_rows, width), jnp.float32)
    for k in range(top_count):
        pick = (dest[:, k : k + 1] == places[None, :]).astype(jnp.bfloat16)
        picked = jnp.dot(pick, came_back, preferred_element_type=jnp.float32)
        combined = combined + picked * gate_weights[:, k : k + 1]
    out_sums = total_over_tp(jnp.sum(combined * combined, axis=1), tp)
    scale_out = lax.rsqrt(out_sums / full_width + epsilon)
    return (combined * scale_out[:, None] * out_gain.astype(jnp.float32)).astype(jnp.bfloat16)


def solution(mesh):
    placed = (
        P("ep", "tp"),
        P("tp"),
        P("ep", None),
        P("ep", None),
        P("ep", None, "tp"),
        P("ep", None, "tp"),
        P("ep", "tp", None),
        P("tp"),
    )

    return jax.shard_map(
        shards, mesh=mesh, in_specs=placed, out_specs=P("ep", "tp"), check_vma=False
    )
```
